512 devices in a mesh: sp: 64 (over z, y), fs: 4 (over x), tp: 2 (over core).
Axes of the slice: x: 4, y: 8, z: 8, core: 2. Of those that a mesh axis runs over, the one named last changes fastest.
Arguments:
- tokens: bfloat16 [16384, 2048], P(('sp', 'fs', 'tp')), may hold values from -6 to 6
- norm_gain: float32 [2048], replicated, may hold values from 0.1 to 1.9
- w_query: bfloat16 [2048, 1024], P(None, ('fs', 'tp')), may hold values from -0.125 to 0.125
- w_key: bfloat16 [2048, 1024], P(None, ('fs', 'tp')), may hold values from -0.125 to 0.125
- w_value: bfloat16 [2048, 1024], P(None, ('fs', 'tp')), may hold values from -0.125 to 0.125
- w_pool: bfloat16 [2048, 1024], P(None, ('fs', 'tp')), may hold values from -0.125 to 0.125
- query_gain: float32 [64], replicated, may hold values from 1.2 to 1.6
- key_gain: float32 [64], replicated, may hold values from 1.2 to 1.6
- lambdas: float32 [8], P(('fs', 'tp')), may hold values from 0.3 to 0.8
- head_gain: float32 [128], replicated, may hold values from 0.1 to 1.9
- w_out_attn: bfloat16 [1024, 2048], P(('fs', 'tp')), may hold values from -0.125 to 0.125
- w_out_pool: bfloat16 [1024, 2048], P(('fs', 'tp')), may hold values from -0.125 to 0.125
Outputs:
- layer_out: bfloat16 [16384, 2048], P(('sp', 'fs', 'tp'))
The draws below stay inside these ranges and needn't reach their ends.
All inputs are finite; a program needn't handle non-finite values.
Results may differ from the reference program's by a relative error of at most 0.015.
Values may be sent and summed in bfloat16 or wider, within the bound.
No kernel may reach another device: no remote copies, remote signals or barrier semaphores. Data moves between devices by JAX's collectives and lax.ppermute only.
A program may use at most 128 MiB of HBM per device.

```python
import math
import jax
import jax.numpy as jnp
from jax import lax

D = 2048
HEADS = 8
HEAD_DIM = 64
V_DIM = 128
ATTN_WIDTH = 1024
POOL_GROUPS = 4
POOL_GROUP_DIM = 256
POOL_WIDTH = 1024
SEQ = 16384


def block_scale(rng, shape, cuts, low, high):
    def one(axis_at, blocks):
        steps = jax.random.uniform(jax.random.fold_in(jax.random.fold_in(rng, 6), axis_at), (blocks,), jnp.float32, low / len(cuts), high / len(cuts))
        return jnp.repeat(jnp.exp(steps), shape[axis_at] // blocks).reshape((-1,) + (1,) * (len(shape) - axis_at - 1))

    level = one(*cuts[0])
    for cut in cuts[1:]:
        level = level * one(*cut)
    return level


def scatter_about(key, extent, spread, most, split=(), kind=jnp.bfloat16):
    entries = spread * jax.random.normal(key, extent, jnp.float32)
    if split:
        entries = entries * block_scale(key, extent, split, -0.22, 0.18)
    return jnp.clip(entries, -most, most).astype(kind)


def setup_inputs(seed: int = 0) -> dict:
    key_list = jax.random.split(jax.random.key(seed), 13)
    return {
        "tokens": scatter_about(key_list[0], (SEQ, D), 1.0, 6.0, ((0, 512),)),
        "norm_gain": jnp.clip(1.0 + 0.18 * jax.random.normal(key_list[1], (D,), jnp.float32), 0.1, 1.9),
        "w_query": scatter_about(key_list[2], (D, HEADS * 2 * HEAD_DIM), D ** -0.5, 0.125, ((1, 8),)),
        "w_key": scatter_about(key_list[3], (D, HEADS * 2 * HEAD_DIM), D ** -0.5, 0.125, ((1, 8),)),
        "w_value": scatter_about(key_list[4], (D, ATTN_WIDTH), D ** -0.5, 0.125, ((1, 8),)),
        "w_pool": scatter_about(key_list[5], (D, POOL_WIDTH), D ** -0.5, 0.125, ((1, 8),)),
        "query_gain": jnp.clip(jax.random.uniform(key_list[6], (HEAD_DIM,), jnp.float32, 1.2, 1.6), 1.2, 1.6),
        "key_gain": jnp.clip(jax.random.uniform(key_list[7], (HEAD_DIM,), jnp.float32, 1.2, 1.6), 1.2, 1.6),
        "lambdas": jnp.clip(0.3 + 0.5 * jax.random.uniform(key_list[8], (HEADS,), jnp.float32) ** block_scale(key_list[8], (HEADS,), ((0, 8),), -0.2, 0.2), 0.3, 0.8),
        "head_gain": jnp.clip(1.0 + 0.18 * jax.random.normal(key_list[9], (V_DIM,), jnp.float32), 0.1, 1.9),
        "w_out_attn": scatter_about(key_list[10], (ATTN_WIDTH, D), (ATTN_WIDTH + POOL_WIDTH) ** -0.5, 0.125, ((0, 8),)),
        "w_out_pool": scatter_about(key_list[11], (POOL_WIDTH, D), (ATTN_WIDTH + POOL_WIDTH) ** -0.5, 0.125, ((0, 8),)),
    }


epsilon = 1e-06
windows = (2, 4, 8, 16)

def rms_scale(values, gain):
    return values * lax.rsqrt(lax.optimization_barrier(jnp.mean(values * values, axis=-1, keepdims=True)) + epsilon) * gain

def attend_head(queries, keys, values, lam_one):
    query_block = math.gcd(SEQ, 512)
    score_scale = HEAD_DIM ** (-0.5)
    key_pos = jnp.arange(SEQ, dtype=jnp.int32)
    keys32 = keys.astype(jnp.float32)
    values32 = values.astype(jnp.float32)
    blocked = queries.reshape(SEQ // query_block, query_block, 2, HEAD_DIM)
    starts = (jnp.arange(SEQ // query_block, dtype=jnp.int32) * query_block).astype(jnp.int32)

    def one_block(inputs):
        query_rows, first_row = inputs
        scores = jnp.einsum('qcd,kcd->cqk', query_rows.astype(jnp.float32), keys32) * score_scale
        query_pos = first_row + jnp.arange(query_block, dtype=jnp.int32)
        visible = key_pos[None, :] <= query_pos[:, None]
        expo = jnp.where(visible[None], jnp.exp(scores), 0.0)
        totals = lax.optimization_barrier(jnp.sum(expo, axis=-1))
        rounded = lax.optimization_barrier(expo.astype(jnp.bfloat16))
        numer = jnp.einsum('cqk,ke->cqe', rounded.astype(jnp.float32), values32)
        return numer[0] / totals[0][:, None] - lam_one * numer[1] / totals[1][:, None]
    head_out = lax.map(one_block, (blocked, starts))
    return head_out.reshape(SEQ, V_DIM)

def pool_mix(pool_input):
    source = pool_input.astype(jnp.float32).reshape(SEQ, POOL_GROUPS, POOL_GROUP_DIM)
    positions = jnp.arange(SEQ, dtype=jnp.float32)
    outputs = []
    for group_index, width_g in enumerate(windows):
        channel = source[:, group_index]
        window_sum = channel
        for offset in range(1, width_g):
            earlier = jnp.concatenate([jnp.zeros((offset, POOL_GROUP_DIM), jnp.float32), channel[:SEQ - offset]], axis=0)
            window_sum = window_sum + earlier
        divisor = jnp.minimum(positions + 1.0, float(width_g))[:, None]
        outputs.append(window_sum / divisor - channel)
    return jnp.stack(outputs, axis=1).reshape(SEQ, POOL_WIDTH).astype(jnp.bfloat16)

def reference(tokens, norm_gain, w_query, w_key, w_value, w_pool, query_gain, key_gain, lambdas, head_gain, w_out_attn, w_out_pool):
    normed = rms_scale(tokens.astype(jnp.float32), norm_gain).astype(jnp.bfloat16)
    query_raw = jnp.dot(normed, w_query, preferred_element_type=jnp.float32).reshape(SEQ, HEADS, 2, HEAD_DIM)
    queries = rms_scale(query_raw, query_gain).astype(jnp.bfloat16)
    key_raw = jnp.dot(normed, w_key, preferred_element_type=jnp.float32).reshape(SEQ, HEADS, 2, HEAD_DIM)
    keys = rms_scale(key_raw, key_gain).astype(jnp.bfloat16)
    values = jnp.dot(normed, w_value, preferred_element_type=jnp.float32).astype(jnp.bfloat16).reshape(SEQ, HEADS, V_DIM)
    pool_input = jnp.dot(normed, w_pool, preferred_element_type=jnp.float32).astype(jnp.bfloat16)

    def per_head(inputs):
        query_h, key_h, value_h, lam_h = inputs
        head_out = attend_head(query_h, key_h, value_h, lam_h)
        return rms_scale(head_out, head_gain).astype(jnp.bfloat16)
    attended = lax.map(per_head, (jnp.transpose(queries, (1, 0, 2, 3)), jnp.transpose(keys, (1, 0, 2, 3)), jnp.transpose(values, (1, 0, 2)), lambdas))
    attended = jnp.transpose(attended, (1, 0, 2)).reshape(SEQ, HEADS * V_DIM)
    pooled = pool_mix(pool_input)
    summed = jnp.dot(attended, w_out_attn, preferred_element_type=jnp.float32) + jnp.dot(pooled, w_out_pool, preferred_element_type=jnp.float32)
    return summed.astype(jnp.bfloat16)
```

```python
import math

import jax
import jax.numpy as jnp
import numpy as np
from jax import lax
from jax.experimental import pallas as pl
from jax.experimental.pallas import tpu as pltpu
from jax.sharding import PartitionSpec as P

EPS = 1e-06
F32 = jnp.float32
BF16 = jnp.bfloat16
DH = 64
SIDE = 8
LANES = 128
EXTRA = 16
VMEM = 56 * 1024 * 1024
SCORE_SCALE = DH**-0.5 * math.log2(math.e)


def params(**kw):
    return pltpu.CompilerParams(vmem_limit_bytes=VMEM, **kw)


def rms_halves(raw, gain):
    left = lax.broadcasted_iota(jnp.int32, raw.shape, 1) < DH
    sq = raw * raw
    a = jnp.sum(jnp.where(left, sq, 0.0), axis=1, keepdims=True) * (1.0 / DH)
    b = jnp.sum(jnp.where(left, 0.0, sq), axis=1, keepdims=True) * (1.0 / DH)
    scale = jnp.where(left, lax.rsqrt(a + EPS), lax.rsqrt(b + EPS))
    return raw * scale * gain


def project_rows(x_ref, g_ref, wqk, wvp, qg_ref, kg_ref):
    chips, rows, width = x_ref.shape
    x = x_ref[...].reshape(chips * rows, width).astype(F32)
    mean = jnp.mean(x * x, axis=1, keepdims=True)
    normed = (x * lax.rsqrt(mean + EPS) * g_ref[...]).astype(BF16)
    qk = jnp.dot(normed, wqk, preferred_element_type=F32)
    vp = jnp.dot(normed, wvp, preferred_element_type=F32)
    twice = lambda ref: jnp.concatenate([ref[...], ref[...]], axis=1)
    q = rms_halves(qk[:, :LANES], twice(qg_ref) * SCORE_SCALE).astype(BF16)
    k = rms_halves(qk[:, LANES:], twice(kg_ref)).astype(BF16)
    return q, k, vp[:, :LANES].astype(BF16), vp[:, LANES:].astype(BF16)


def own_kernel(x_ref, g_ref, wq_ref, wk_ref, wv_ref, wp_ref, qg_ref, kg_ref, wqk_ref, wvp_ref, half_ref):
    wqk_ref[:, :LANES] = wq_ref[...]
    wqk_ref[:, LANES:] = wk_ref[...]
    wvp_ref[:, :LANES] = wv_ref[...]
    wvp_ref[:, LANES:] = wp_ref[...]
    parts = project_rows(x_ref, g_ref, wqk_ref[...], wvp_ref[...], qg_ref, kg_ref)
    for n, part in enumerate(parts):
        half_ref[n] = part


def far_kernel(core_ref, x_ref, half_ref, g_ref, wqk_ref, wvp_ref, qg_ref, kg_ref, q_ref, kv_ref, p_ref):
    chips, rows, _ = x_ref.shape
    copies = q_ref.shape[0]
    core = core_ref[0]
    far = project_rows(x_ref, g_ref, wqk_ref[...], wvp_ref[...], qg_ref, kg_ref)
    own = tuple(half_ref[n] for n in range(4))
    for (q, k, v, p), side in ((own, core), (far, 1 - core)):
        for i in range(chips):
            src = slice(i * rows, (i + 1) * rows)
            dst = pl.ds(pl.multiple_of((i * 2 + side) * rows, rows), rows)
            p_ref[dst, :] = p[src]
            for n in range(copies):
                q_ref[n, dst, :] = q[src]
                kv_ref[n, dst, :LANES] = k[src]
                kv_ref[n, dst, LANES:] = v[src]


def attend_kernel(at_ref, q_ref, kv_ref, o_ref, v1_ref, p_ref):
    blocks, rows, _ = kv_ref.shape
    for j in range(blocks):
        v1_ref[pl.ds(j * rows, rows), :LANES] = kv_ref[j, :, LANES:]
        v1_ref[pl.ds(j * rows, rows), LANES:] = jnp.ones((rows, LANES), BF16)
    k_first = at_ref[2]
    k_step = at_ref[3]

    def attend(i, q_block, count):
        q = q_ref[i]
        left = lax.broadcasted_iota(jnp.int32, q.shape, 1) < DH
        zero = jnp.zeros_like(q)
        q2 = jnp.concatenate([jnp.where(left, q, zero), jnp.where(left, zero, q)], axis=0)
        row = lax.broadcasted_iota(jnp.int32, (2 * rows, rows), 0) % rows
        ahead = lax.broadcasted_iota(jnp.int32, (2 * rows, rows), 1) - row
        for j in range(count):
            s = lax.dot_general(
                q2, kv_ref[j, :, :LANES], (((1,), (1,)), ((), ())), preferred_element_type=F32
            )
            room = (q_block - (k_first + k_step * j)) * rows
            p_ref[:, pl.ds(j * rows, rows)] = jnp.where(ahead <= room, jnp.exp2(s), 0.0).astype(BF16)
        out = jnp.dot(
            p_ref[:, : count * rows], v1_ref[: count * rows], preferred_element_type=F32
        )
        o_ref[i, :rows, :LANES] = out[:rows, :LANES].astype(BF16)
        o_ref[i, :rows, LANES:] = out[rows:, :LANES].astype(BF16)
        eye = lax.broadcasted_iota(jnp.int32, (LANES, LANES), 0) == lax.broadcasted_iota(
            jnp.int32, (LANES, LANES), 1
        )
        line = lax.broadcasted_iota(jnp.int32, (EXTRA, LANES), 0)
        for half in range(rows // LANES):
            tail = jnp.zeros((EXTRA, LANES), F32)
            for m in range(2):
                at = m * rows + half * LANES
                tot = out[at : at + LANES, LANES:]
                tot = jnp.sum(jnp.where(eye, tot, 0.0), axis=0, keepdims=True)
                high = tot.astype(BF16).astype(F32)
                tail = jnp.where(line == 2 * m, high, tail)
                tail = jnp.where(line == 2 * m + 1, tot - high, tail)
            o_ref[i, rows:, half * LANES : (half + 1) * LANES] = tail.astype(BF16)

    def one(i, carry):
        q_block = at_ref[0] + at_ref[1] * i
        many = k_first + k_step * (blocks // 2) <= q_block
        some = k_first <= q_block

        @pl.when(many)
        def _():
            attend(i, q_block, blocks)

        @pl.when(jnp.logical_and(some, jnp.logical_not(many)))
        def _():
            attend(i, q_block, blocks // 2)

        @pl.when(jnp.logical_not(some))
        def _():
            o_ref[i] = jnp.zeros(o_ref.shape[1:], BF16)

        return carry

    lax.fori_loop(0, o_ref.shape[0], one, 0)


def finish_kernel(at_ref, lam_ref, r_ref, pool_ref, halo_ref, hg_ref, wa_ref, wp_ref, keep_ref, send_ref, ext_ref, mix_ref):
    sources = r_ref.shape[0]
    chips, part, _ = keep_ref.shape
    rows = 2 * chips * part
    total = r_ref[0].astype(F32)
    for n in range(1, sources):
        total = total + r_ref[n].astype(F32)
    eye = lax.broadcasted_iota(jnp.int32, (LANES, LANES), 0) == lax.broadcasted_iota(
        jnp.int32, (LANES, LANES), 1
    )

    def column(m):
        cols = []
        for half in range(rows // LANES):
            at = slice(half * LANES, (half + 1) * LANES)
            line = total[rows + 2 * m : rows + 2 * m + 1, at] + total[rows + 2 * m + 1 : rows + 2 * m + 2, at]
            cols.append(jnp.sum(jnp.where(eye, line, 0.0), axis=1, keepdims=True))
        return jnp.concatenate(cols, axis=0)

    head = total[:rows, :LANES] / column(0) - lam_ref[0] * (total[:rows, LANES:] / column(1))
    mean = jnp.mean(head * head, axis=1, keepdims=True)
    attended = (head * lax.rsqrt(mean + EPS) * hg_ref[...]).astype(BF16)

    window = at_ref[1]
    halo = halo_ref.shape[0]
    ext_ref[:halo, :] = jnp.zeros((halo, LANES), F32)
    ext_ref[halo : 2 * halo, :] = halo_ref[...].astype(F32)
    ext_ref[2 * halo :, :] = pool_ref[...].astype(F32)
    pick = ext_ref[2 * halo :, :]
    own = pick
    span = 1
    total_rows = rows + 2 * halo
    while span < halo:
        wider = ext_ref[halo:, :] + ext_ref[halo - span : total_rows - span, :]
        ext_ref[halo:, :] = wider
        span *= 2
        pick = jnp.where(window == span, wider[halo:, :], pick)
    pos = at_ref[0] * rows + lax.broadcasted_iota(jnp.int32, (rows, LANES), 0)
    divisor = jnp.minimum(pos + 1, window).astype(F32)
    pooled = (pick / divisor - own).astype(BF16)

    mix_ref[:, :LANES] = attended
    mix_ref[:, LANES:] = pooled
    weights = jnp.concatenate([wa_ref[...], wp_ref[...]], axis=0)
    core = at_ref[2]
    for ref, side in ((send_ref, 1 - core), (keep_ref, core)):
        picked = [
            mix_ref[pl.ds(pl.multiple_of((n * 2 + side) * part, part), part), :] for n in range(chips)
        ]
        out = jnp.dot(jnp.concatenate(picked, axis=0), weights, preferred_element_type=F32)
        ref[...] = out.astype(BF16).reshape(ref.shape)


def plane_groups():
    index = np.arange(SIDE * SIDE * 2).reshape(SIDE, SIDE, 2)
    along_y = [[index[z, :, c].tolist() for z in range(SIDE)] for c in range(2)]
    along_z = [[index[:, y, c].tolist() for y in range(SIDE)] for c in range(2)]
    return along_y[0] + along_z[1], along_z[0] + along_y[1]


KEY_GROUPS, QUERY_GROUPS = plane_groups()


def in_vmem(x):
    return pltpu.with_memory_space_constraint(x, pltpu.VMEM)


def exchange(x, groups):
    return lax.all_to_all(
        x, ("sp", "tp"), split_axis=0, concat_axis=0, axis_index_groups=groups, tiled=True
    )


def body(
    tokens,
    norm_gain,
    w_query,
    w_key,
    w_value,
    w_pool,
    query_gain,
    key_gain,
    lambdas,
    head_gain,
    w_out_attn,
    w_out_pool,
):
    part, width = tokens.shape
    chips, cores = lax.axis_size("fs"), lax.axis_size("tp")
    rows = part * chips * cores
    place = lax.axis_index("sp")
    core = lax.axis_index("tp")
    z, y = place // SIDE, place % SIDE

    near = lax.all_gather(tokens, "fs", axis=0)
    far = lax.ppermute(near, "tp", [(0, 1), (1, 0)])

    vm = pl.BlockSpec(memory_space=pltpu.VMEM)
    sm = pl.BlockSpec(memory_space=pltpu.SMEM)
    here = core.astype(jnp.int32)[None]
    gains = (query_gain[None], key_gain[None])
    wqk, wvp, half = pl.pallas_call(
        own_kernel,
        in_specs=[vm] * 8,
        out_specs=[vm] * 3,
        out_shape=[
            pltpu.VMEM((width, 2 * LANES), BF16),
            pltpu.VMEM((width, 2 * LANES), BF16),
            pltpu.VMEM((4, chips * part, LANES), BF16),
        ],
        compiler_params=params(),
        name="own",
    )(in_vmem(near), norm_gain[None], w_query, w_key, w_value, w_pool, *gains)
    queries, keyvals, pool_input = pl.pallas_call(
        far_kernel,
        in_specs=[sm] + [vm] * 7,
        out_specs=[vm] * 3,
        out_shape=[
            pltpu.VMEM((SIDE, rows, LANES), BF16),
            pltpu.VMEM((SIDE, rows, 2 * LANES), BF16),
            pltpu.VMEM((rows, LANES), BF16),
        ],
        compiler_params=params(),
        name="far",
    )(here, in_vmem(far), in_vmem(half), norm_gain[None], in_vmem(wqk), in_vmem(wvp), *gains)

    devices = lax.axis_size("sp")
    halo = lax.ppermute(pool_input[rows - 16 :], "sp", [(i, i + 1) for i in range(devices - 1)])
    keyvals = exchange(keyvals, KEY_GROUPS)
    queries = exchange(queries, QUERY_GROUPS)

    across = core == 0
    where_at = jnp.stack(
        [
            jnp.where(across, y, SIDE * z),
            jnp.where(across, SIDE, 1),
            jnp.where(across, SIDE * z, y),
            jnp.where(across, 1, SIDE),
        ]
    ).astype(jnp.int32)
    partial = pl.pallas_call(
        attend_kernel,
        in_specs=[sm, vm, vm],
        out_specs=vm,
        out_shape=pltpu.VMEM((SIDE, rows + EXTRA, 2 * LANES), BF16),
        scratch_shapes=[
            pltpu.VMEM((SIDE * rows, 2 * LANES), BF16),
            pltpu.VMEM((2 * rows, SIDE * rows), BF16),
        ],
        compiler_params=params(),
        name="attend",
    )(where_at, in_vmem(queries), in_vmem(keyvals))

    partial = exchange(partial, QUERY_GROUPS)

    spot = jnp.stack([place, 2 << lax.axis_index("fs"), core]).astype(jnp.int32)
    keep, send = pl.pallas_call(
        finish_kernel,
        in_specs=[sm, sm] + [vm] * 6,
        out_specs=[vm, vm],
        out_shape=[pltpu.VMEM((chips, part, width), BF16)] * 2,
        scratch_shapes=[
            pltpu.VMEM((rows + 32, LANES), F32),
            pltpu.VMEM((rows, 2 * LANES), BF16),
        ],
        compiler_params=params(),
        name="finish",
    )(
        spot,
        lambdas,
        in_vmem(partial),
        in_vmem(pool_input),
        in_vmem(halo),
        head_gain[None],
        in_vmem(w_out_attn),
        in_vmem(w_out_pool),
    )

    other = lax.ppermute(send, "tp", [(0, 1), (1, 0)])
    mixed = (keep.astype(F32) + other.astype(F32)).astype(BF16)
    mixed = lax.all_to_all(mixed, "fs", split_axis=0, concat_axis=0, tiled=True)
    return jnp.sum(mixed.astype(F32), axis=0).astype(BF16)


def solution(mesh):
    return jax.shard_map(
        body,
        mesh=mesh,
        in_specs=(
            P(("sp", "fs", "tp"), None),
            P(),
            P(None, ("fs", "tp")),
            P(None, ("fs", "tp")),
            P(None, ("fs", "tp")),
            P(None, ("fs", "tp")),
            P(),
            P(),
            P(("fs", "tp")),
            P(),
            P(("fs", "tp"), None),
            P(("fs", "tp"), None),
        ),
        out_specs=P(("sp", "fs", "tp"), None),
        check_vma=False,
    )
```

```python
import math

import jax
import jax.numpy as jnp
import numpy as np
from jax import lax
from jax.experimental import pallas as pl
from jax.experimental.pallas import tpu as pltpu
from jax.sharding import PartitionSpec as P


EPS = 1e-06
F32 = jnp.float32
BF16 = jnp.bfloat16
DH = 64
SIDE = 8
LANES = 128
EXTRA = 16
VMEM = 56 * 1024 * 1024
SCORE_SCALE = DH**-0.5 * math.log2(math.e)


def params(**kw):
    return pltpu.CompilerParams(vmem_limit_bytes=VMEM, **kw)


def rms_halves(raw, gain):
    left = lax.broadcasted_iota(jnp.int32, raw.shape, 1) < DH
    sq = raw * raw
    a = jnp.sum(jnp.where(left, sq, 0.0), axis=1, keepdims=True) * (1.0 / DH)
    b = jnp.sum(jnp.where(left, 0.0, sq), axis=1, keepdims=True) * (1.0 / DH)
    scale = jnp.where(left, lax.rsqrt(a + EPS), lax.rsqrt(b + EPS))
    return raw * scale * gain


def project_rows(x_ref, g_ref, wqk, wvp, qg_ref, kg_ref):
    chips, rows, width = x_ref.shape
    x = x_ref[...].reshape(chips * rows, width).astype(F32)
    mean = jnp.mean(x * x, axis=1, keepdims=True)
    normed = (x * lax.rsqrt(mean + EPS) * g_ref[...]).astype(BF16)
    qk = jnp.dot(normed, wqk, preferred_element_type=F32)
    vp = jnp.dot(normed, wvp, preferred_element_type=F32)
    twice = lambda ref: jnp.concatenate([ref[...], ref[...]], axis=1)
    q = rms_halves(qk[:, :LANES], twice(qg_ref) * SCORE_SCALE).astype(BF16)
    k = rms_halves(qk[:, LANES:], twice(kg_ref)).astype(BF16)
    return q, k, vp[:, :LANES].astype(BF16), vp[:, LANES:].astype(BF16)


def own_kernel(x_ref, g_ref, wq_ref, wk_ref, wv_ref, wp_ref, qg_ref, kg_ref, wqk_ref, wvp_ref, half_ref):
    wqk_ref[:, :LANES] = wq_ref[...]
    wqk_ref[:, LANES:] = wk_ref[...]
    wvp_ref[:, :LANES] = wv_ref[...]
    wvp_ref[:, LANES:] = wp_ref[...]
    parts = project_rows(x_ref, g_ref, wqk_ref[...], wvp_ref[...], qg_ref, kg_ref)
    for n, part in enumerate(parts):
        half_ref[n] = part


def far_kernel(core_ref, x_ref, half_ref, g_ref, wqk_ref, wvp_ref, qg_ref, kg_ref, q_ref, kv_ref, p_ref):
    chips, rows, _ = x_ref.shape
    copies = kv_ref.shape[0]
    core = core_ref[0]
    far = project_rows(x_ref, g_ref, wqk_ref[...], wvp_ref[...], qg_ref, kg_ref)
    own = tuple(half_ref[n] for n in range(4))
    for (q, k, v, p), side in ((own, core), (far, 1 - core)):
        for i in range(chips):
            src = slice(i * rows, (i + 1) * rows)
            dst = pl.ds(pl.multiple_of((i * 2 + side) * rows, rows), rows)
            p_ref[dst, :] = p[src]
            q_ref[dst, :] = q[src]
            for n in range(copies):
                kv_ref[n, dst, :LANES] = k[src]
                kv_ref[n, dst, LANES:] = v[src]


def attend_kernel(at_ref, q_ref, kv_ref, o_ref, v1_ref, p_ref):
    blocks, rows, _ = kv_ref.shape
    for j in range(blocks):
        v1_ref[pl.ds(j * rows, rows), :LANES] = kv_ref[j, :, LANES:]
        v1_ref[pl.ds(j * rows, rows), LANES:] = jnp.ones((rows, LANES), BF16)
    k_first = at_ref[2]
    k_step = at_ref[3]

    def attend(step, i, q_block, count):
        q = q_ref[step]
        left = lax.broadcasted_iota(jnp.int32, q.shape, 1) < DH
        zero = jnp.zeros_like(q)
        q2 = jnp.concatenate([jnp.where(left, q, zero), jnp.where(left, zero, q)], axis=0)
        row = lax.broadcasted_iota(jnp.int32, (2 * rows, rows), 0) % rows
        ahead = lax.broadcasted_iota(jnp.int32, (2 * rows, rows), 1) - row
        for j in range(count):
            s = lax.dot_general(
                q2, kv_ref[j, :, :LANES], (((1,), (1,)), ((), ())), preferred_element_type=F32
            )
            room = (q_block - (k_first + k_step * j)) * rows
            p_ref[:, pl.ds(j * rows, rows)] = jnp.where(ahead <= room, jnp.exp2(s), 0.0).astype(BF16)
        out = jnp.dot(
            p_ref[:, : count * rows], v1_ref[: count * rows], preferred_element_type=F32
        )
        o_ref[i, :rows, :LANES] = out[:rows, :LANES].astype(BF16)
        o_ref[i, :rows, LANES:] = out[rows:, :LANES].astype(BF16)
        eye = lax.broadcasted_iota(jnp.int32, (LANES, LANES), 0) == lax.broadcasted_iota(
            jnp.int32, (LANES, LANES), 1
        )
        line = lax.broadcasted_iota(jnp.int32, (EXTRA, LANES), 0)
        for half in range(rows // LANES):
            tail = jnp.zeros((EXTRA, LANES), F32)
            for m in range(2):
                at = m * rows + half * LANES
                tot = out[at : at + LANES, LANES:]
                tot = jnp.sum(jnp.where(eye, tot, 0.0), axis=0, keepdims=True)
                high = tot.astype(BF16).astype(F32)
                tail = jnp.where(line == 2 * m, high, tail)
                tail = jnp.where(line == 2 * m + 1, tot - high, tail)
            o_ref[i, rows:, half * LANES : (half + 1) * LANES] = tail.astype(BF16)

    def one(step, carry):
        odd = step % 2
        i = step - odd + jnp.where(at_ref[4] == 1, 1 - odd, odd)
        q_block = at_ref[0] + at_ref[1] * i
        many = k_first + k_step * (blocks // 2) <= q_block
        some = k_first <= q_block

        @pl.when(many)
        def _():
            attend(step, i, q_block, blocks)

        @pl.when(jnp.logical_and(some, jnp.logical_not(many)))
        def _():
            attend(step, i, q_block, blocks // 2)

        @pl.when(jnp.logical_not(some))
        def _():
            o_ref[i] = jnp.zeros(o_ref.shape[1:], BF16)

        return carry

    lax.fori_loop(0, o_ref.shape[0], one, 0)


def finish_kernel(at_ref, lam_ref, r_ref, pool_ref, halo_ref, hg_ref, wa_ref, wp_ref, keep_ref, send_ref, ext_ref, mix_ref):
    sources = r_ref.shape[0]
    chips, part, _ = keep_ref.shape
    rows = 2 * chips * part
    total = r_ref[0].astype(F32)
    for n in range(1, sources):
        total = total + r_ref[n].astype(F32)
    eye = lax.broadcasted_iota(jnp.int32, (LANES, LANES), 0) == lax.broadcasted_iota(
        jnp.int32, (LANES, LANES), 1
    )

    def column(m):
        cols = []
        for half in range(rows // LANES):
            at = slice(half * LANES, (half + 1) * LANES)
            line = total[rows + 2 * m : rows + 2 * m + 1, at] + total[rows + 2 * m + 1 : rows + 2 * m + 2, at]
            cols.append(jnp.sum(jnp.where(eye, line, 0.0), axis=1, keepdims=True))
        return jnp.concatenate(cols, axis=0)

    head = total[:rows, :LANES] / column(0) - lam_ref[0] * (total[:rows, LANES:] / column(1))
    mean = jnp.mean(head * head, axis=1, keepdims=True)
    attended = (head * lax.rsqrt(mean + EPS) * hg_ref[...]).astype(BF16)

    window = at_ref[1]
    halo = halo_ref.shape[0]
    ext_ref[:halo, :] = jnp.zeros((halo, LANES), F32)
    ext_ref[halo : 2 * halo, :] = halo_ref[...].astype(F32)
    ext_ref[2 * halo :, :] = pool_ref[...].astype(F32)
    pick = ext_ref[2 * halo :, :]
    own = pick
    span = 1
    total_rows = rows + 2 * halo
    while span < halo:
        wider = ext_ref[halo:, :] + ext_ref[halo - span : total_rows - span, :]
        ext_ref[halo:, :] = wider
        span *= 2
        pick = jnp.where(window == span, wider[halo:, :], pick)
    pos = at_ref[0] * rows + lax.broadcasted_iota(jnp.int32, (rows, LANES), 0)
    divisor = jnp.minimum(pos + 1, window).astype(F32)
    pooled = (pick / divisor - own).astype(BF16)

    mix_ref[:, :LANES] = attended
    mix_ref[:, LANES:] = pooled
    weights = jnp.concatenate([wa_ref[...], wp_ref[...]], axis=0)
    core = at_ref[2]
    for ref, side in ((send_ref, 1 - core), (keep_ref, core)):
        picked = [
            mix_ref[pl.ds(pl.multiple_of((n * 2 + side) * part, part), part), :] for n in range(chips)
        ]
        out = jnp.dot(jnp.concatenate(picked, axis=0), weights, preferred_element_type=F32)
        ref[...] = out.astype(BF16).reshape(ref.shape)


def plane_groups():
    index = np.arange(SIDE * SIDE * 2).reshape(SIDE, SIDE, 2)
    along_y = [[index[z, :, c].tolist() for z in range(SIDE)] for c in range(2)]
    along_z = [[index[:, y, c].tolist() for y in range(SIDE)] for c in range(2)]
    return along_y[0] + along_z[1], along_z[0] + along_y[1]


KEY_GROUPS, QUERY_GROUPS = plane_groups()
QUERY_PAIRS = [(g[i], g[i ^ 1]) for g in QUERY_GROUPS for i in range(SIDE)]
QUERY_FOURS = [g[parity::2] for g in QUERY_GROUPS for parity in range(2)]


def in_vmem(x):
    return pltpu.with_memory_space_constraint(x, pltpu.VMEM)


def exchange(x, groups):
    return lax.all_to_all(
        x, ("sp", "tp"), split_axis=0, concat_axis=0, axis_index_groups=groups, tiled=True
    )


def body(
    tokens,
    norm_gain,
    w_query,
    w_key,
    w_value,
    w_pool,
    query_gain,
    key_gain,
    lambdas,
    head_gain,
    w_out_attn,
    w_out_pool,
):
    part, width = tokens.shape
    chips, cores = lax.axis_size("fs"), lax.axis_size("tp")
    rows = part * chips * cores
    place = lax.axis_index("sp")
    core = lax.axis_index("tp")
    z, y = place // SIDE, place % SIDE

    near = lax.all_gather(tokens, "fs", axis=0)
    far = lax.ppermute(near, "tp", [(0, 1), (1, 0)])

    vm = pl.BlockSpec(memory_space=pltpu.VMEM)
    sm = pl.BlockSpec(memory_space=pltpu.SMEM)
    here = core.astype(jnp.int32)[None]
    gains = (query_gain[None], key_gain[None])
    wqk, wvp, half = pl.pallas_call(
        own_kernel,
        in_specs=[vm] * 8,
        out_specs=[vm] * 3,
        out_shape=[
            pltpu.VMEM((width, 2 * LANES), BF16),
            pltpu.VMEM((width, 2 * LANES), BF16),
            pltpu.VMEM((4, chips * part, LANES), BF16),
        ],
        compiler_params=params(),
        name="own",
    )(in_vmem(near), norm_gain[None], w_query, w_key, w_value, w_pool, *gains)
    queries, keyvals, pool_input = pl.pallas_call(
        far_kernel,
        in_specs=[sm] + [vm] * 7,
        out_specs=[vm] * 3,
        out_shape=[
            pltpu.VMEM((rows, LANES), BF16),
            pltpu.VMEM((SIDE, rows, 2 * LANES), BF16),
            pltpu.VMEM((rows, LANES), BF16),
        ],
        compiler_params=params(),
        name="far",
    )(here, in_vmem(far), in_vmem(half), norm_gain[None], in_vmem(wqk), in_vmem(wvp), *gains)

    devices = lax.axis_size("sp")
    halo = lax.ppermute(pool_input[rows - 16 :], "sp", [(i, i + 1) for i in range(devices - 1)])
    keyvals = exchange(keyvals, KEY_GROUPS)
    beside = lax.ppermute(queries, ("sp", "tp"), QUERY_PAIRS)
    queries = jnp.stack([queries, beside])
    queries = lax.all_gather(queries, ("sp", "tp"), axis=0, axis_index_groups=QUERY_FOURS, tiled=True)

    across = core == 0
    where_at = jnp.stack(
        [
            jnp.where(across, y, SIDE * z),
            jnp.where(across, SIDE, 1),
            jnp.where(across, SIDE * z, y),
            jnp.where(across, 1, SIDE),
            jnp.where(across, z, y) % 2,
        ]
    ).astype(jnp.int32)
    partial = pl.pallas_call(
        attend_kernel,
        in_specs=[sm, vm, vm],
        out_specs=vm,
        out_shape=pltpu.VMEM((SIDE, rows + EXTRA, 2 * LANES), BF16),
        scratch_shapes=[
            pltpu.VMEM((SIDE * rows, 2 * LANES), BF16),
            pltpu.VMEM((2 * rows, SIDE * rows), BF16),
        ],
        compiler_params=params(),
        name="attend",
    )(where_at, in_vmem(queries), in_vmem(keyvals))

    partial = exchange(partial, QUERY_GROUPS)

    spot = jnp.stack([place, 2 << lax.axis_index("fs"), core]).astype(jnp.int32)
    keep, send = pl.pallas_call(
        finish_kernel,
        in_specs=[sm, sm] + [vm] * 6,
        out_specs=[vm, vm],
        out_shape=[pltpu.VMEM((chips, part, width), BF16)] * 2,
        scratch_shapes=[
            pltpu.VMEM((rows + 32, LANES), F32),
            pltpu.VMEM((rows, 2 * LANES), BF16),
        ],
        compiler_params=params(),
        name="finish",
    )(
        spot,
        lambdas,
        in_vmem(partial),
        in_vmem(pool_input),
        in_vmem(halo),
        head_gain[None],
        in_vmem(w_out_attn),
        in_vmem(w_out_pool),
    )

    other = lax.ppermute(send, "tp", [(0, 1), (1, 0)])
    mixed = (keep.astype(F32) + other.astype(F32)).astype(BF16)
    mixed = lax.all_to_all(mixed, "fs", split_axis=0, concat_axis=0, tiled=True)
    return jnp.sum(mixed.astype(F32), axis=0).astype(BF16)


def solution(mesh):
    return jax.shard_map(
        body,
        mesh=mesh,
        in_specs=(
            P(("sp", "fs", "tp"), None),
            P(),
            P(None, ("fs", "tp")),
            P(None, ("fs", "tp")),
            P(None, ("fs", "tp")),
            P(None, ("fs", "tp")),
            P(),
            P(),
            P(("fs", "tp")),
            P(),
            P(("fs", "tp"), None),
            P(("fs", "tp"), None),
        ),
        out_specs=P(("sp", "fs", "tp"), None),
        check_vma=False,
    )
```

```python
import math

import jax
import jax.numpy as jnp
import numpy as np
from jax import lax
from jax.experimental import pallas as pl
from jax.experimental.pallas import tpu as pltpu
from jax.sharding import PartitionSpec as P


EPS = 1e-06
F32 = jnp.float32
BF16 = jnp.bfloat16
DH = 64
SIDE = 8
LANES = 128
EXTRA = 16
VMEM = 56 * 1024 * 1024
SCORE_SCALE = DH**-0.5 * math.log2(math.e)


def params(**kw):
    return pltpu.CompilerParams(vmem_limit_bytes=VMEM, **kw)


def rms_halves(raw, gain):
    left = lax.broadcasted_iota(jnp.int32, raw.shape, 1) < DH
    sq = raw * raw
    a = jnp.sum(jnp.where(left, sq, 0.0), axis=1, keepdims=True) * (1.0 / DH)
    b = jnp.sum(jnp.where(left, 0.0, sq), axis=1, keepdims=True) * (1.0 / DH)
    scale = jnp.where(left, lax.rsqrt(a + EPS), lax.rsqrt(b + EPS))
    return raw * scale * gain


def project_rows(x_ref, g_ref, wqk, wvp, qg_ref, kg_ref):
    chips, rows, width = x_ref.shape
    x = x_ref[...].reshape(chips * rows, width).astype(F32)
    mean = jnp.mean(x * x, axis=1, keepdims=True)
    normed = (x * lax.rsqrt(mean + EPS) * g_ref[...]).astype(BF16)
    qk = jnp.dot(normed, wqk, preferred_element_type=F32)
    vp = jnp.dot(normed, wvp, preferred_element_type=F32)
    twice = lambda ref: jnp.concatenate([ref[...], ref[...]], axis=1)
    q = rms_halves(qk[:, :LANES], twice(qg_ref) * SCORE_SCALE).astype(BF16)
    k = rms_halves(qk[:, LANES:], twice(kg_ref)).astype(BF16)
    return q, k, vp[:, :LANES].astype(BF16), vp[:, LANES:].astype(BF16)


def own_kernel(x_ref, g_ref, wq_ref, wk_ref, wv_ref, wp_ref, qg_ref, kg_ref, wqk_ref, wvp_ref, half_ref):
    wqk_ref[:, :LANES] = wq_ref[...]
    wqk_ref[:, LANES:] = wk_ref[...]
    wvp_ref[:, :LANES] = wv_ref[...]
    wvp_ref[:, LANES:] = wp_ref[...]
    parts = project_rows(x_ref, g_ref, wqk_ref[...], wvp_ref[...], qg_ref, kg_ref)
    for n, part in enumerate(parts):
        half_ref[n] = part


def far_kernel(core_ref, x_ref, half_ref, g_ref, wqk_ref, wvp_ref, qg_ref, kg_ref, q_ref, kv_ref, p_ref):
    chips, rows, _ = x_ref.shape
    copies = kv_ref.shape[0]
    core = core_ref[0]
    far = project_rows(x_ref, g_ref, wqk_ref[...], wvp_ref[...], qg_ref, kg_ref)
    own = tuple(half_ref[n] for n in range(4))
    for (q, k, v, p), side in ((own, core), (far, 1 - core)):
        for i in range(chips):
            src = slice(i * rows, (i + 1) * rows)
            dst = pl.ds(pl.multiple_of((i * 2 + side) * rows, rows), rows)
            p_ref[dst, :] = p[src]
            q_ref[dst, :] = q[src]
            for n in range(copies):
                kv_ref[n, dst, :LANES] = k[src]
                kv_ref[n, dst, LANES:] = v[src]


def early_kernel(at_ref, q_ref, kv_ref, o_ref, v1_ref, *held):
    blocks, rows, _ = kv_ref.shape
    for j in range(blocks):
        v1_ref[pl.ds(j * rows, rows), :LANES] = kv_ref[j, :, LANES:]
        v1_ref[pl.ds(j * rows, rows), LANES:] = jnp.ones((rows, LANES), BF16)
    attend_half(1, at_ref, q_ref, kv_ref, o_ref, v1_ref, held)


def late_kernel(at_ref, q_ref, kv_ref, v1_ref, o_ref, *held):
    attend_half(0, at_ref, q_ref, kv_ref, o_ref, v1_ref, held)


def merge_kernel(a_ref, b_ref, o_ref):
    blocks, rows, _ = o_ref.shape
    rows -= EXTRA
    line = lax.broadcasted_iota(jnp.int32, (EXTRA, 2 * LANES), 0)
    for n in range(blocks):
        o_ref[n, :rows] = (a_ref[n, :rows].astype(F32) + b_ref[n, :rows].astype(F32)).astype(BF16)
        both = a_ref[n, rows:].astype(F32) + b_ref[n, rows:].astype(F32)
        tail = jnp.zeros((EXTRA, 2 * LANES), F32)
        for m in range(2):
            tot = both[2 * m : 2 * m + 1] + both[2 * m + 1 : 2 * m + 2]
            high = tot.astype(BF16).astype(F32)
            tail = jnp.where(line == 2 * m, high, tail)
            tail = jnp.where(line == 2 * m + 1, tot - high, tail)
        o_ref[n, rows:] = tail.astype(BF16)


def attend_half(other, at_ref, q_ref, kv_ref, o_ref, v1_ref, held):
    blocks, rows, _ = kv_ref.shape
    tall = 2 * rows
    k_first = at_ref[2]
    k_step = at_ref[3]

    def score(i, p_ref):
        q_block = at_ref[0] + at_ref[1] * (2 * i + jnp.where(at_ref[4] == 1, 1 - other, other))
        q = q_ref[2 * i + other]
        left = lax.broadcasted_iota(jnp.int32, q.shape, 1) < DH
        zero = jnp.zeros_like(q)
        q2 = jnp.concatenate([jnp.where(left, q, zero), jnp.where(left, zero, q)], axis=0)
        row = lax.broadcasted_iota(jnp.int32, (tall, rows), 0) % rows
        ahead = lax.broadcasted_iota(jnp.int32, (tall, rows), 1) - row
        for j in range(blocks):
            s = lax.dot_general(
                q2, kv_ref[j, :, :LANES], (((1,), (1,)), ((), ())), preferred_element_type=F32
            )
            room = (q_block - (k_first + k_step * j)) * rows
            p_ref[:, pl.ds(j * rows, rows)] = jnp.where(
                ahead <= room, jnp.exp2(s), 0.0
            ).astype(BF16)

    def gather(i, p_ref):
        out = jnp.dot(p_ref[...], v1_ref[...], preferred_element_type=F32)
        o_ref[i, :rows, :LANES] = out[:rows, :LANES].astype(BF16)
        o_ref[i, :rows, LANES:] = out[rows:, :LANES].astype(BF16)
        eye = lax.broadcasted_iota(jnp.int32, (LANES, LANES), 0) == lax.broadcasted_iota(
            jnp.int32, (LANES, LANES), 1
        )
        line = lax.broadcasted_iota(jnp.int32, (EXTRA, LANES), 0)
        for half in range(rows // LANES):
            tail = jnp.zeros((EXTRA, LANES), F32)
            for m in range(2):
                at = m * rows + half * LANES
                tot = out[at : at + LANES, LANES:]
                tot = jnp.sum(jnp.where(eye, tot, 0.0), axis=0, keepdims=True)
                high = tot.astype(BF16).astype(F32)
                tail = jnp.where(line == 2 * m, high, tail)
                tail = jnp.where(line == 2 * m + 1, tot - high, tail)
            o_ref[i, rows:, half * LANES : (half + 1) * LANES] = tail.astype(BF16)

    count = o_ref.shape[0]

    def span(begin):
        score(begin, held[0])
        for i in range(begin, count):
            if i + 1 < count:
                score(i + 1, held[(i - begin + 1) % 2])
            gather(i, held[(i - begin) % 2])

    unseen = k_first > at_ref[0] + at_ref[1] * (count - 1)

    @pl.when(unseen)
    def _():
        o_ref[: count // 2] = jnp.zeros((count // 2, *o_ref.shape[1:]), BF16)
        span(count // 2)

    @pl.when(jnp.logical_not(unseen))
    def _():
        span(0)


def finish_kernel(at_ref, lam_ref, r_ref, pool_ref, halo_ref, hg_ref, mix_ref, ext_ref):
    sources = r_ref.shape[0]
    rows = mix_ref.shape[0]
    total = r_ref[0].astype(F32)
    for n in range(1, sources):
        total = total + r_ref[n].astype(F32)
    eye = lax.broadcasted_iota(jnp.int32, (LANES, LANES), 0) == lax.broadcasted_iota(
        jnp.int32, (LANES, LANES), 1
    )

    def column(m):
        cols = []
        for half in range(rows // LANES):
            at = slice(half * LANES, (half + 1) * LANES)
            line = total[rows + 2 * m : rows + 2 * m + 1, at] + total[rows + 2 * m + 1 : rows + 2 * m + 2, at]
            cols.append(jnp.sum(jnp.where(eye, line, 0.0), axis=1, keepdims=True))
        return jnp.concatenate(cols, axis=0)

    head = total[:rows, :LANES] / column(0) - lam_ref[0] * (total[:rows, LANES:] / column(1))
    mean = jnp.mean(head * head, axis=1, keepdims=True)
    attended = (head * lax.rsqrt(mean + EPS) * hg_ref[...]).astype(BF16)

    window = at_ref[6]
    halo = halo_ref.shape[0]
    ext_ref[:halo, :] = jnp.zeros((halo, LANES), F32)
    ext_ref[halo : 2 * halo, :] = halo_ref[...].astype(F32)
    ext_ref[2 * halo :, :] = pool_ref[...].astype(F32)
    pick = ext_ref[2 * halo :, :]
    own = pick
    span = 1
    total_rows = rows + 2 * halo
    while span < halo:
        wider = ext_ref[halo:, :] + ext_ref[halo - span : total_rows - span, :]
        ext_ref[halo:, :] = wider
        span *= 2
        pick = jnp.where(window == span, wider[halo:, :], pick)
    pos = at_ref[5] * rows + lax.broadcasted_iota(jnp.int32, (rows, LANES), 0)
    divisor = jnp.minimum(pos + 1, window).astype(F32)
    pooled = (pick / divisor - own).astype(BF16)

    mix_ref[:, :LANES] = attended
    mix_ref[:, LANES:] = pooled


def output_kernel(at_ref, mix_ref, wa_ref, wp_ref, far_wa_ref, far_wp_ref, o_ref):
    chips, part, _ = o_ref.shape
    core = at_ref[7]

    def product(side, attn, pool):
        rows = jnp.concatenate(
            [
                mix_ref[side, pl.ds(pl.multiple_of((n * 2 + core) * part, part), part), :]
                for n in range(chips)
            ],
            axis=0,
        )
        weights = jnp.concatenate([attn[...], pool[...]], axis=0)
        return jnp.dot(rows, weights, preferred_element_type=F32)

    out = product(core, wa_ref, wp_ref) + product(1 - core, far_wa_ref, far_wp_ref)
    o_ref[...] = out.astype(BF16).reshape(o_ref.shape)


def plane_groups():
    index = np.arange(SIDE * SIDE * 2).reshape(SIDE, SIDE, 2)
    along_y = [[index[z, :, c].tolist() for z in range(SIDE)] for c in range(2)]
    along_z = [[index[:, y, c].tolist() for y in range(SIDE)] for c in range(2)]
    return along_y[0] + along_z[1], along_z[0] + along_y[1]


KEY_GROUPS, QUERY_GROUPS = plane_groups()
QUERY_PAIRS = [(g[i], g[i ^ 1]) for g in QUERY_GROUPS for i in range(SIDE)]
QUERY_FOURS = [g[parity::2] for g in QUERY_GROUPS for parity in range(2)]


def in_vmem(x):
    return pltpu.with_memory_space_constraint(x, pltpu.VMEM)


def exchange(x, groups):
    return lax.all_to_all(
        x, ("sp", "tp"), split_axis=0, concat_axis=0, axis_index_groups=groups, tiled=True
    )


def body(
    tokens,
    norm_gain,
    w_query,
    w_key,
    w_value,
    w_pool,
    query_gain,
    key_gain,
    lambdas,
    head_gain,
    w_out_attn,
    w_out_pool,
):
    part, width = tokens.shape
    chips, cores = lax.axis_size("fs"), lax.axis_size("tp")
    rows = part * chips * cores
    place = lax.axis_index("sp")
    core = lax.axis_index("tp")
    z, y = place // SIDE, place % SIDE

    near = lax.all_gather(tokens, "fs", axis=0)
    far = lax.ppermute(near, "tp", [(0, 1), (1, 0)])

    vm = pl.BlockSpec(memory_space=pltpu.VMEM)
    sm = pl.BlockSpec(memory_space=pltpu.SMEM)
    here = core.astype(jnp.int32)[None]
    gains = (query_gain[None], key_gain[None])
    wqk, wvp, half = pl.pallas_call(
        own_kernel,
        in_specs=[vm] * 8,
        out_specs=[vm] * 3,
        out_shape=[
            pltpu.VMEM((width, 2 * LANES), BF16),
            pltpu.VMEM((width, 2 * LANES), BF16),
            pltpu.VMEM((4, chips * part, LANES), BF16),
        ],
        compiler_params=params(),
        name="own",
    )(in_vmem(near), norm_gain[None], w_query, w_key, w_value, w_pool, *gains)
    queries, keyvals, pool_input = pl.pallas_call(
        far_kernel,
        in_specs=[sm] + [vm] * 7,
        out_specs=[vm] * 3,
        out_shape=[
            pltpu.VMEM((rows, LANES), BF16),
            pltpu.VMEM((SIDE, rows, 2 * LANES), BF16),
            pltpu.VMEM((rows, LANES), BF16),
        ],
        compiler_params=params(),
        name="far",
    )(here, in_vmem(far), in_vmem(half), norm_gain[None], in_vmem(wqk), in_vmem(wvp), *gains)

    devices = lax.axis_size("sp")
    halo = lax.ppermute(pool_input[rows - 16 :], "sp", [(i, i + 1) for i in range(devices - 1)])
    keyvals = exchange(keyvals, KEY_GROUPS)
    beside = lax.ppermute(queries, ("sp", "tp"), QUERY_PAIRS)
    queries = jnp.stack([queries, beside])
    queries = lax.all_gather(queries, ("sp", "tp"), axis=0, axis_index_groups=QUERY_FOURS, tiled=True)

    across = core == 0
    where_at = jnp.stack(
        [
            jnp.where(across, y, SIDE * z),
            jnp.where(across, SIDE, 1),
            jnp.where(across, SIDE * z, y),
            jnp.where(across, 1, SIDE),
            jnp.where(across, z, y) % 2,
            place,
            2 << lax.axis_index("fs"),
            core,
        ]
    ).astype(jnp.int32)
    half_shape = pltpu.VMEM((SIDE // 2, rows + EXTRA, 2 * LANES), BF16)
    weights_scratch = pltpu.VMEM((2 * rows, SIDE * rows), BF16)
    queries, keyvals = in_vmem(queries), in_vmem(keyvals)
    early, values_ones = pl.pallas_call(
        early_kernel,
        in_specs=[sm, vm, vm],
        out_specs=[vm, vm],
        out_shape=[half_shape, pltpu.VMEM((SIDE * rows, 2 * LANES), BF16)],
        scratch_shapes=[weights_scratch] * 2,
        compiler_params=params(),
        name="early",
    )(where_at, queries, keyvals)
    passed = lax.ppermute(early, ("sp", "tp"), QUERY_PAIRS)
    late = pl.pallas_call(
        late_kernel,
        in_specs=[sm, vm, vm, vm],
        out_specs=vm,
        out_shape=half_shape,
        scratch_shapes=[weights_scratch] * 2,
        compiler_params=params(),
        name="late",
    )(where_at, queries, keyvals, in_vmem(values_ones))
    partial = pl.pallas_call(
        merge_kernel,
        in_specs=[vm, vm],
        out_specs=vm,
        out_shape=half_shape,
        compiler_params=params(),
        name="merge",
    )(in_vmem(late), in_vmem(passed))
    partial = exchange(partial, QUERY_FOURS)
    far_attn = lax.ppermute(w_out_attn, "tp", [(0, 1), (1, 0)])
    far_pool = lax.ppermute(w_out_pool, "tp", [(0, 1), (1, 0)])

    mixed = pl.pallas_call(
        finish_kernel,
        in_specs=[sm, sm] + [vm] * 4,
        out_specs=vm,
        out_shape=pltpu.VMEM((rows, 2 * LANES), BF16),
        scratch_shapes=[pltpu.VMEM((rows + 32, LANES), F32)],
        compiler_params=params(),
        name="finish",
    )(
        where_at,
        lambdas,
        in_vmem(partial),
        in_vmem(pool_input),
        in_vmem(halo),
        head_gain[None],
    )
    mixed = lax.all_gather(mixed, "tp", axis=0)
    mixed = pl.pallas_call(
        output_kernel,
        in_specs=[sm] + [vm] * 5,
        out_specs=vm,
        out_shape=pltpu.VMEM((chips, part, width), BF16),
        compiler_params=params(),
        name="output",
    )(where_at, in_vmem(mixed), *map(in_vmem, (w_out_attn, w_out_pool, far_attn, far_pool)))
    mixed = lax.all_to_all(mixed, "fs", split_axis=0, concat_axis=0, tiled=True)
    return jnp.sum(mixed.astype(F32), axis=0).astype(BF16)


def solution(mesh):
    return jax.shard_map(
        body,
        mesh=mesh,
        in_specs=(
            P(("sp", "fs", "tp"), None),
            P(),
            P(None, ("fs", "tp")),
            P(None, ("fs", "tp")),
            P(None, ("fs", "tp")),
            P(None, ("fs", "tp")),
            P(),
            P(),
            P(("fs", "tp")),
            P(),
            P(("fs", "tp"), None),
            P(("fs", "tp"), None),
        ),
        out_specs=P(("sp", "fs", "tp"), None),
        check_vma=False,
    )
```
